32 devices in a mesh: rep: 2 (over x), fs: 8 (over z, y), tp: 2 (over core).
Axes of the slice: x: 2, y: 2, z: 4, core: 2. Of those that a mesh axis runs over, the one named last changes fastest.
Arguments:
- later_input: bfloat16 [2048, 2048], P(('rep', 'fs')), may hold values from -6 to 6
- earlier_input: bfloat16 [2048, 2048], P(('rep', 'fs')), may hold values from -6 to 6
- cotangent: bfloat16 [2048, 2048], P(('rep', 'fs')), may hold values from -6 to 6
- gate_weight: bfloat16 [2048, 3072], P('fs', 'tp'), may hold values from -0.125 to 0.125
- up_weight: bfloat16 [2048, 3072], P('fs', 'tp'), may hold values from -0.125 to 0.125
- down_weight: bfloat16 [2048, 3072], P('fs', 'tp'), may hold values from -0.109375 to 0.109375
- gate_sum: float32 [2048, 3072], P('fs', 'tp'), may hold values from -192 to 192
- up_sum: float32 [2048, 3072], P('fs', 'tp'), may hold values from -192 to 192
- down_sum: float32 [2048, 3072], P('fs', 'tp'), may hold values from -192 to 192
Outputs:
- later_output: bfloat16 [2048, 2048], P(('rep', 'fs'))
- earlier_input_grad: bfloat16 [2048, 2048], P(('rep', 'fs'))
- gate_sum_new: float32 [2048, 3072], P('fs', 'tp')
- up_sum_new: float32 [2048, 3072], P('fs', 'tp')
- down_sum_new: float32 [2048, 3072], P('fs', 'tp')
The draws below stay inside these ranges and needn't reach their ends.
All inputs are finite; a program needn't handle non-finite values.
Results may differ from the reference program's by a relative error of at most 0.02.
Values may be sent and summed in bfloat16 or wider, within the bound.
A program may use at most 128 MiB of HBM per device.

```python
import jax
import jax.numpy as jnp
from jax import lax

D = 2048
FF = 3072
TOKENS = 2048
N_TP = 2


def with_spikes(values, rng, source, target, blocks, factor):
    owner, partner = [(jnp.arange(values.shape[dim]) // (values.shape[dim] // blocks)).reshape([-1 if axis == dim else 1 for axis in range(values.ndim)]) for dim in (source, target)]
    chosen = jax.random.permutation(rng, blocks)[partner]
    strong = (owner == chosen) | (owner == (partner + blocks // 2) % blocks)
    return jnp.where(strong, factor * values, values)


def block_scale(key, extent, shards, smallest, largest):
    factor_of = 1.0
    for dim, parts in shards:
        heights = jax.random.uniform(jax.random.fold_in(jax.random.fold_in(key, 6), dim), (parts,), jnp.float32, smallest / len(shards), largest / len(shards))
        factor_of = factor_of * jnp.repeat(jnp.exp(heights), extent[dim] // parts).reshape((-1,) + (1,) * (len(extent) - 1 - dim))
    return factor_of


def normal_values(own_key, extent, scale, limit, pieces=(), kind=jnp.bfloat16):
    entries = scale * jax.random.normal(own_key, extent, jnp.float32)
    if pieces:
        entries = entries * block_scale(own_key, extent, pieces, -0.22, 0.18)
    return jnp.clip(entries, -limit, limit).astype(kind)


def bell_draw_with(rng, dims, scale, reach, split, heavy, held_as=jnp.bfloat16):
    values = scale * jax.random.normal(rng, dims, jnp.float32)
    if split:
        values = values * block_scale(rng, dims, split, -0.22, 0.18)
    return jnp.clip(with_spikes(values, jax.random.fold_in(rng, 3), *heavy), -reach, reach).astype(held_as)


def setup_inputs(seed: int = 0) -> dict:
    arg_keys = jax.random.split(jax.random.key(seed), 10)
    return {
        "later_input": normal_values(arg_keys[0], (TOKENS, D), 1.0, 6.0, ((0, 16),)),
        "earlier_input": normal_values(arg_keys[1], (TOKENS, D), 1.0, 6.0, ((0, 16),)),
        "cotangent": bell_draw_with(arg_keys[2], (TOKENS, D), 1.0, 6.0, ((0, 16),), (0, 1, 16, 2.0)),
        "gate_weight": normal_values(arg_keys[3], (D, FF), D ** -0.5, 0.125, ((0, 8), (1, 2))),
        "up_weight": normal_values(arg_keys[4], (D, FF), D ** -0.5, 0.125, ((0, 8), (1, 2))),
        "down_weight": normal_values(arg_keys[5], (D, FF), FF ** -0.5, 0.109375, ((0, 8), (1, 2))),
        "gate_sum": normal_values(arg_keys[6], (D, FF), 32.0, 192.0, ((0, 8), (1, 2)), jnp.float32),
        "up_sum": normal_values(arg_keys[7], (D, FF), 32.0, 192.0, ((0, 8), (1, 2)), jnp.float32),
        "down_sum": normal_values(arg_keys[8], (D, FF), 32.0, 192.0, ((0, 8), (1, 2)), jnp.float32),
    }


def contract_last(first, second):
    return lax.dot_general(first, second, (((1,), (1,)), ((), ())), preferred_element_type=jnp.float32)


def contract_first(first, second):
    return lax.dot_general(first, second, (((0,), (0,)), ((), ())), preferred_element_type=jnp.float32)


def blockwise(firsts, seconds):
    block_width = FF // N_TP
    running = jnp.zeros((firsts[0].shape[0], seconds[0].shape[0]), jnp.float32)
    for block_index in range(N_TP):
        lower = block_index * block_width
        partial_value = jnp.zeros_like(running)
        for first, second in zip(firsts, seconds):
            partial_value = partial_value + contract_last(first[:, lower:lower + block_width], second[:, lower:lower + block_width])
        rounded = lax.optimization_barrier(partial_value.astype(jnp.bfloat16))
        running = running + rounded.astype(jnp.float32)
    return running.astype(jnp.bfloat16)


def reference(later_input, earlier_input, cotangent, gate_weight, up_weight, down_weight, gate_sum, up_sum, down_sum):
    gate_late = jnp.dot(later_input, gate_weight, preferred_element_type=jnp.float32)
    up_late = jnp.dot(later_input, up_weight, preferred_element_type=jnp.float32)
    hidden_late = (jax.nn.silu(gate_late) * up_late).astype(jnp.bfloat16)
    later_output = blockwise([hidden_late], [down_weight])
    gate_early = jnp.dot(earlier_input, gate_weight, preferred_element_type=jnp.float32)
    up_early = jnp.dot(earlier_input, up_weight, preferred_element_type=jnp.float32)
    hidden_grad = jnp.dot(cotangent, down_weight, preferred_element_type=jnp.float32)
    sigmoid_gate = jax.nn.sigmoid(gate_early)
    silu_early = gate_early * sigmoid_gate
    gate_grad = (hidden_grad * up_early * sigmoid_gate * (1.0 + gate_early * (1.0 - sigmoid_gate))).astype(jnp.bfloat16)
    up_grad = (hidden_grad * silu_early).astype(jnp.bfloat16)
    hidden_early = (silu_early * up_early).astype(jnp.bfloat16)
    earlier_input_grad = blockwise([gate_grad, up_grad], [gate_weight, up_weight])
    gate_sum_new = gate_sum + contract_first(earlier_input, gate_grad)
    up_sum_new = up_sum + contract_first(earlier_input, up_grad)
    down_sum_new = down_sum + contract_first(cotangent, hidden_early)
    return later_output, earlier_input_grad, gate_sum_new, up_sum_new, down_sum_new
```

```python
import functools

import jax
import jax.numpy as jnp
from jax import lax
from jax.experimental import pallas as pl
from jax.experimental.pallas import tpu as pltpu
from jax.sharding import PartitionSpec as P

MESH = pl.DeviceIdType.MESH


def ring_position(index, n):
    side, height = lax.rem(index, 2), index // 2
    return (1 - side) * height + side * (n - 1 - height)


def ring_index(position, n):
    position = lax.rem(position + 2 * n, n)
    back = position // (n // 2)
    return (1 - back) * (2 * position) + back * (2 * (n - 1 - position) + 1)


def span(start, size, step):
    return pl.ds(pl.multiple_of(start, step), size)


def remote(source, target, send, recv, device):
    return pltpu.make_async_remote_copy(
        src_ref=source,
        dst_ref=target,
        send_sem=send,
        recv_sem=recv,
        device_id=device,
        device_id_type=MESH,
    )


def meet(n, r, f, t):
    barrier = pltpu.get_barrier_semaphore()
    for k in range(1, n):
        pl.semaphore_signal(barrier, inc=1, device_id={"fs": lax.rem(f + k, n)}, device_id_type=MESH)
    pl.semaphore_signal(barrier, inc=1, device_id={"rep": 1 - r}, device_id_type=MESH)
    pl.semaphore_signal(barrier, inc=1, device_id={"tp": 1 - t}, device_id_type=MESH)
    pl.semaphore_wait(barrier, n + 1)


def gather_kernel(n, tok, wt, tok_out, w_out, rs, rr, ps, pr, ws, wr, xs, xr):
    r, f, t = lax.axis_index("rep"), lax.axis_index("fs"), lax.axis_index("tp")
    m = tok.shape[1]
    q = m // 4
    hid, dl = wt.shape[1] // n, wt.shape[2]
    hl = dl // 2
    pos = ring_position(f, n)
    ahead = (ring_index(pos + 1, n), ring_index(pos - 1, n))
    meet(n, r, f, t)

    def rows(origin, core, d):
        return tok_out.at[:, span(origin * m + core * (2 * q) + d * q, q, q), :]

    def piece(origin, part):
        return w_out.at[:, :, span(origin * dl + part * hl, hl, hl)]

    pending = []
    for d in range(2):
        copy = remote(
            tok.at[:, span(t * (2 * q) + d * q, q, q), :],
            rows(f, t, d), rs.at[d, 0], rr.at[d, 0], {"fs": ahead[d]},
        )
        copy.start()
        pending.append(copy)
    for k in range(1, n):
        g = lax.rem(f + k, n)
        copy = remote(
            wt.at[:, span(g * hid, hid, hid), span(r * hl, hl, hl)],
            piece(f, r), ws.at[k - 1], wr.at[k - 1], {"fs": g},
        )
        copy.start()
        pending.append(copy)
    tok_out[:, span(f * m, m, m), :] = tok[...]
    w_out[:, :, span(f * dl, dl, dl)] = wt[:, span(f * hid, hid, hid), :]

    arrivals = []
    for s in range(1, n):
        for d in range(2):
            origin = ring_index(pos - s if d == 0 else pos + s, n)
            block = rows(origin, t, d)
            remote(block, block, rs.at[d, s - 1], rr.at[d, s - 1], {"fs": ahead[d]}).wait_recv()
            if s < n - 1:
                copy = remote(block, block, rs.at[d, s], rr.at[d, s], {"fs": ahead[d]})
                copy.start()
                pending.append(copy)
            copy = remote(block, block, ps.at[d, s - 1], pr.at[d, s - 1], {"tp": 1 - t})
            copy.start()
            pending.append(copy)
            other = rows(origin, 1 - t, d)
            arrivals.append(remote(other, other, ps.at[d, s - 1], pr.at[d, s - 1], {"tp": 1 - t}))
        origin = lax.rem(f - s + n, n)
        block = piece(origin, r)
        remote(block, block, ws.at[s - 1], wr.at[s - 1], {"fs": origin}).wait_recv()
        copy = remote(block, block, xs.at[s - 1], xr.at[s - 1], {"rep": 1 - r})
        copy.start()
        pending.append(copy)
        other = piece(origin, 1 - r)
        arrivals.append(remote(other, other, xs.at[s - 1], xr.at[s - 1], {"rep": 1 - r}))
    for copy in arrivals:
        copy.wait_recv()
    for copy in pending:
        copy.wait_send()


def scatter_kernel(
    n, late, early, grads, late_out, early_out, g_out,
    peer, ring_in, ring_out, x_in, x_out,
    ts, tr, rs, rr, os_, or_, xs, xr, gs, gr, fs_, fr,
):
    r, f, t = lax.axis_index("rep"), lax.axis_index("fs"), lax.axis_index("tp")
    m = late.shape[1]
    q = m // 4
    hid = grads.shape[1]
    dl = grads.shape[2] // n
    hl = dl // 2
    pos = ring_position(f, n)
    ahead = (ring_index(pos + 1, n), ring_index(pos - 1, n))
    parts, outs = (late, early), (late_out, early_out)
    f32 = jnp.float32
    meet(n, r, f, t)

    pending = []

    def go(copy):
        copy.start()
        pending.append(copy)

    for o in range(2):
        go(remote(parts[o].at[:, span((1 - t) * (2 * q), 2 * q, 2 * q), :], peer.at[o], ts.at[o], tr.at[o], {"tp": 1 - t}))
    order = list(range(1, n)) + [0]
    for k in order:
        g = lax.rem(f + k, n)
        go(remote(grads.at[:, :, span(g * dl + (1 - r) * hl, hl, hl)], x_in.at[k], xs.at[k], xr.at[k], {"rep": 1 - r}))

    def own(o, b, d):
        return (
            parts[o][b, span(t * (2 * q) + d * q, q, q), :].astype(f32)
            + peer[o, b, d * q:(d + 1) * q, :].astype(f32)
        )

    def g_block(origin, part):
        return g_out.at[:, span(origin * hid, hid, hid), span(part * hl, hl, hl)]

    def pair_sum(k):
        g = lax.rem(f + k, n)
        remote(x_in.at[k], x_in.at[k], xs.at[k], xr.at[k], {"rep": 1 - r}).wait_recv()
        return (x_in[k].astype(f32) + grads[:, :, span(g * dl + r * hl, hl, hl)].astype(f32)).astype(jnp.bfloat16)

    def pass_on(k):
        origin = lax.rem(f - k + n, n)
        block = g_block(origin, r)
        remote(block, block, gs.at[k - 1], gr.at[k - 1], {"fs": origin}).wait_recv()
        go(remote(block, block, fs_.at[k], fr.at[k], {"rep": 1 - r}))

    for s in range(n - 1):
        for o in range(2):
            if s == 0:
                remote(peer.at[o], peer.at[o], ts.at[o], tr.at[o], {"tp": 1 - t}).wait_recv()
            for d in range(2):
                b = ring_index(pos - 1 - s if d == 0 else pos + 1 + s, n)
                value = own(o, b, d)
                if s > 0:
                    slot = ring_in.at[d, s - 1, o]
                    remote(slot, slot, rs.at[d, s - 1, o], rr.at[d, s - 1, o], {"fs": ahead[d]}).wait_recv()
                    value = value + ring_in[d, s - 1, o].astype(f32)
                ring_out[d, s, o] = value.astype(jnp.bfloat16)
                go(remote(ring_out.at[d, s, o], ring_in.at[d, s, o], rs.at[d, s, o], rr.at[d, s, o], {"fs": ahead[d]}))
        x_out[s] = pair_sum(s + 1)
        go(remote(x_out.at[s], g_block(f, r), gs.at[s], gr.at[s], {"fs": lax.rem(f + s + 1, n)}))
        if s >= 2:
            pass_on(s - 1)
    g_out[:, span(f * hid, hid, hid), span(r * hl, hl, hl)] = pair_sum(0)
    block = g_block(f, r)
    go(remote(block, block, fs_.at[0], fr.at[0], {"rep": 1 - r}))
    for o in range(2):
        for d in range(2):
            slot = ring_in.at[d, n - 2, o]
            remote(slot, slot, rs.at[d, n - 2, o], rr.at[d, n - 2, o], {"fs": ahead[d]}).wait_recv()
            value = own(o, f, d) + ring_in[d, n - 2, o].astype(f32)
            outs[o][span(t * (2 * q) + d * q, q, q), :] = value.astype(jnp.bfloat16)
        half = outs[o].at[span(t * (2 * q), 2 * q, 2 * q), :]
        go(remote(half, half, os_.at[o], or_.at[o], {"tp": 1 - t}))
    for k in range(n - 2, n):
        pass_on(k)
    for o in range(2):
        half = outs[o].at[span((1 - t) * (2 * q), 2 * q, 2 * q), :]
        remote(half, half, os_.at[o], or_.at[o], {"tp": 1 - t}).wait_recv()
    for k in range(n):
        block = g_block(lax.rem(f - k + n, n), 1 - r)
        remote(block, block, fs_.at[k], fr.at[k], {"rep": 1 - r}).wait_recv()
    for copy in pending:
        copy.wait_send()


VMEM = pl.BlockSpec(memory_space=pltpu.VMEM)


def dma(*shape):
    return pltpu.SemaphoreType.DMA(shape)


def split_hidden(
    n,
    later_input,
    earlier_input,
    cotangent,
    gate_weight,
    up_weight,
    down_weight,
    gate_sum,
    up_sum,
    down_sum,
):
    bf16 = jnp.bfloat16
    m, width = later_input.shape
    dl, ff = gate_weight.shape
    hid = ff // n
    hl, q = dl // 2, m // 4
    tokens = jnp.stack([later_input, earlier_input, cotangent])
    weights = jnp.stack([gate_weight.T, up_weight.T, down_weight.T])
    tok, w = pl.pallas_call(
        functools.partial(gather_kernel, n),
        out_shape=(
            jax.ShapeDtypeStruct((3, n * m, width), bf16),
            jax.ShapeDtypeStruct((3, hid, width), bf16),
        ),
        in_specs=[VMEM] * 2,
        out_specs=(VMEM, VMEM),
        scratch_shapes=[dma(2, n - 1)] * 4 + [dma(n - 1)] * 4,
        compiler_params=pltpu.CompilerParams(
            collective_id=0, has_side_effects=True, vmem_limit_bytes=60 * 1024 * 1024
        ),
        name="gather",
    )(tokens, weights)
    count = n * m
    both = tok[:2].reshape(2 * count, width)
    gate, up = contract_last(both, w[0]), contract_last(both, w[1])
    hidden_late = (jax.nn.silu(gate[:count]) * up[:count]).astype(bf16)
    late = jnp.dot(hidden_late, w[2], preferred_element_type=jnp.float32).astype(bf16)
    gate_early, up_early = gate[count:], up[count:]
    hidden_grad = contract_last(tok[2], w[2])
    gate_grad, up_grad, hidden_early = early_parts(gate_early, up_early, hidden_grad)
    early = (
        jnp.dot(gate_grad, w[0], preferred_element_type=jnp.float32)
        + jnp.dot(up_grad, w[1], preferred_element_type=jnp.float32)
    ).astype(bf16)
    grads = jnp.stack([
        contract_first(gate_grad, tok[1]).astype(bf16),
        contract_first(up_grad, tok[1]).astype(bf16),
        contract_first(hidden_early, tok[2]).astype(bf16),
    ])
    later_output, earlier_input_grad, total = pl.pallas_call(
        functools.partial(scatter_kernel, n),
        out_shape=(
            jax.ShapeDtypeStruct((m, width), bf16),
            jax.ShapeDtypeStruct((m, width), bf16),
            jax.ShapeDtypeStruct((3, ff, dl), bf16),
        ),
        in_specs=[VMEM] * 3,
        out_specs=(VMEM, VMEM, VMEM),
        scratch_shapes=[
            pltpu.VMEM((2, n, 2 * q, width), bf16),
            pltpu.VMEM((2, n - 1, 2, q, width), bf16),
            pltpu.VMEM((2, n - 1, 2, q, width), bf16),
            pltpu.VMEM((n, 3, hid, hl), bf16),
            pltpu.VMEM((n - 1, 3, hid, hl), bf16),
            dma(2), dma(2),
            dma(2, n - 1, 2), dma(2, n - 1, 2),
            dma(2), dma(2),
            dma(n), dma(n),
            dma(n - 1), dma(n - 1),
            dma(n), dma(n),
        ],
        compiler_params=pltpu.CompilerParams(
            collective_id=1, has_side_effects=True, vmem_limit_bytes=60 * 1024 * 1024
        ),
        name="scatter",
    )(late.reshape(n, m, width), early.reshape(n, m, width), grads)
    return (
        later_output,
        earlier_input_grad,
        gate_sum + total[0].T.astype(jnp.float32),
        up_sum + total[1].T.astype(jnp.float32),
        down_sum + total[2].T.astype(jnp.float32),
    )


def early_parts(gate_early, up_early, hidden_grad):
    sigmoid_gate = jax.nn.sigmoid(gate_early)
    silu_early = gate_early * sigmoid_gate
    gate_grad = (
        hidden_grad * up_early * sigmoid_gate * (1.0 + gate_early * (1.0 - sigmoid_gate))
    ).astype(jnp.bfloat16)
    up_grad = (hidden_grad * silu_early).astype(jnp.bfloat16)
    hidden_early = (silu_early * up_early).astype(jnp.bfloat16)
    return gate_grad, up_grad, hidden_early


def contract_last(first, second):
    return lax.dot_general(
        first, second, (((1,), (1,)), ((), ())), preferred_element_type=jnp.float32
    )


def contract_first(first, second):
    return lax.dot_general(
        first, second, (((0,), (0,)), ((), ())), preferred_element_type=jnp.float32
    )


def per_device(
    later_input,
    earlier_input,
    cotangent,
    gate_weight,
    up_weight,
    down_weight,
    gate_sum,
    up_sum,
    down_sum,
):
    gate_full, up_full, down_full = (
        lax.all_gather(gate_weight, "fs", axis=0, tiled=True),
        lax.all_gather(up_weight, "fs", axis=0, tiled=True),
        lax.all_gather(down_weight, "fs", axis=0, tiled=True),
    )
    gate_late = jnp.dot(later_input, gate_full, preferred_element_type=jnp.float32)
    up_late = jnp.dot(later_input, up_full, preferred_element_type=jnp.float32)
    hidden_late = (jax.nn.silu(gate_late) * up_late).astype(jnp.bfloat16)
    partial_late = contract_last(hidden_late, down_full)
    later_output = lax.psum(partial_late.astype(jnp.bfloat16), "tp")
    gate_early = jnp.dot(earlier_input, gate_full, preferred_element_type=jnp.float32)
    up_early = jnp.dot(earlier_input, up_full, preferred_element_type=jnp.float32)
    hidden_grad = jnp.dot(cotangent, down_full, preferred_element_type=jnp.float32)
    sigmoid_gate = jax.nn.sigmoid(gate_early)
    silu_early = gate_early * sigmoid_gate
    gate_grad = (
        hidden_grad * up_early * sigmoid_gate * (1.0 + gate_early * (1.0 - sigmoid_gate))
    ).astype(jnp.bfloat16)
    up_grad = (hidden_grad * silu_early).astype(jnp.bfloat16)
    hidden_early = (silu_early * up_early).astype(jnp.bfloat16)
    partial_early = contract_last(gate_grad, gate_full) + contract_last(up_grad, up_full)
    earlier_input_grad = lax.psum(partial_early.astype(jnp.bfloat16), "tp")
    columns, cot_columns = (
        lax.all_to_all(earlier_input, "fs", split_axis=1, concat_axis=0, tiled=True),
        lax.all_to_all(cotangent, "fs", split_axis=1, concat_axis=0, tiled=True),
    )
    gate_local = contract_first(columns, lax.all_gather(gate_grad, "fs", axis=0, tiled=True))
    up_local = contract_first(columns, lax.all_gather(up_grad, "fs", axis=0, tiled=True))
    down_local = contract_first(cot_columns, lax.all_gather(hidden_early, "fs", axis=0, tiled=True))
    gate_total, up_total, down_total = (
        lax.psum(gate_local.astype(jnp.bfloat16), "rep").astype(jnp.float32),
        lax.psum(up_local.astype(jnp.bfloat16), "rep").astype(jnp.float32),
        lax.psum(down_local.astype(jnp.bfloat16), "rep").astype(jnp.float32),
    )
    return (
        later_output,
        earlier_input_grad,
        gate_sum + gate_total,
        up_sum + up_total,
        down_sum + down_total,
    )


def solution(mesh):
    placed = (
        P(("rep", "fs"), None),
        P(("rep", "fs"), None),
        P(("rep", "fs"), None),
        P("fs", "tp"),
        P("fs", "tp"),
        P("fs", "tp"),
        P("fs", "tp"),
        P("fs", "tp"),
        P("fs", "tp"),
    )
    reps, shards, blocks = (mesh.shape[axis] for axis in ("rep", "fs", "tp"))

    def chosen(*arrays):
        rows = arrays[0].shape[0]
        depth, units = arrays[3].shape
        fits = (
            reps == 2
            and blocks == 2
            and shards % 2 == 0
            and units % (shards * 16) == 0
            and depth % 256 == 0
            and rows % 64 == 0
        )
        return split_hidden(shards, *arrays) if fits else per_device(*arrays)

    return jax.shard_map(
        chosen,
        mesh=mesh,
        in_specs=placed,
        out_specs=(
            P(("rep", "fs"), None),
            P(("rep", "fs"), None),
            P("fs", "tp"),
            P("fs", "tp"),
            P("fs", "tp"),
        ),
        check_vma=False,
    )
```

```python
import functools

import jax
import jax.numpy as jnp
from jax import lax
from jax.experimental import pallas as pl
from jax.experimental.pallas import tpu as pltpu
from jax.sharding import PartitionSpec as P

MESH = pl.DeviceIdType.MESH


def ring_position(index, n):
    side, height = lax.rem(index, 2), index // 2
    return (1 - side) * height + side * (n - 1 - height)


def ring_index(position, n):
    position = lax.rem(position + 2 * n, n)
    back = position // (n // 2)
    return (1 - back) * (2 * position) + back * (2 * (n - 1 - position) + 1)


def span(start, size, step):
    return pl.ds(pl.multiple_of(start, step), size)


def remote(source, target, send, recv, device):
    return pltpu.make_async_remote_copy(
        src_ref=source,
        dst_ref=target,
        send_sem=send,
        recv_sem=recv,
        device_id=device,
        device_id_type=MESH,
    )


def meet(n, r, f, t):
    barrier = pltpu.get_barrier_semaphore()
    for k in range(1, n):
        pl.semaphore_signal(barrier, inc=1, device_id={"fs": lax.rem(f + k, n)}, device_id_type=MESH)
    pl.semaphore_signal(barrier, inc=1, device_id={"rep": 1 - r}, device_id_type=MESH)
    pl.semaphore_signal(barrier, inc=1, device_id={"tp": 1 - t}, device_id_type=MESH)
    pl.semaphore_wait(barrier, n + 1)


def fused_kernel(
    n, tok, wt, late_out, early_out, g_out,
    slots, w, part, peer, acc, grads, ring_in, ring_out, x_in, x_out,
    ags, agr, aps, apr, ws, wr, wxs, wxr,
    ts, tr, rs, rr, os_, or_, xs, xr, gs, gr, fs_, fr,
):
    r, f, t = lax.axis_index("rep"), lax.axis_index("fs"), lax.axis_index("tp")
    m = tok.shape[1]
    q = m // 4
    hid, dl = wt.shape[1] // n, wt.shape[2]
    hl = dl // 2
    width = tok.shape[2]
    pos = ring_position(f, n)
    ahead = (ring_index(pos + 1, n), ring_index(pos - 1, n))
    outs = (late_out, early_out)
    f32, bf16 = jnp.float32, jnp.bfloat16
    meet(n, r, f, t)

    pending = []

    def go(copy):
        copy.start()
        pending.append(copy)

    def quarter(core, d):
        return span(core * (2 * q) + d * q, q, q)

    def half(core):
        return span(core * (2 * q), 2 * q, 2 * q)

    def piece(origin, side):
        return w.at[:, :, span(origin * dl + side * hl, hl, hl)]

    for k in range(1, n):
        g = lax.rem(f + k, n)
        go(remote(
            wt.at[:, span(g * hid, hid, hid), span(r * hl, hl, hl)],
            piece(f, r), ws.at[k - 1], wr.at[k - 1], {"fs": g},
        ))
    for d in range(2):
        go(remote(tok.at[:, quarter(t, d), :], slots.at[1, :, quarter(t, d), :], ags.at[d, 0], agr.at[d, 0], {"fs": ahead[d]}))
    slots[0] = tok[...]
    w[:, :, span(f * dl, dl, dl)] = wt[:, span(f * hid, hid, hid), :]
    acc[...] = jnp.zeros_like(acc)
    for k in range(1, n):
        origin = lax.rem(f - k + n, n)
        block = piece(origin, r)
        remote(block, block, ws.at[k - 1], wr.at[k - 1], {"fs": origin}).wait_recv()
        go(remote(block, block, wxs.at[k - 1], wxr.at[k - 1], {"rep": 1 - r}))
    for k in range(1, n):
        block = piece(lax.rem(f - k + n, n), 1 - r)
        remote(block, block, wxs.at[k - 1], wxr.at[k - 1], {"rep": 1 - r}).wait_recv()

    step = width // 4

    def compute(s):
        pair = slots[s, 0:2].reshape(2 * m, width)
        gate, up = contract_last(pair, w[0]), contract_last(pair, w[1])
        hidden_late = (jax.nn.silu(gate[:m]) * up[:m]).astype(bf16)
        hidden_grad = contract_last(slots[s, 2], w[2])
        gate_grad, up_grad, hidden_early = early_parts(gate[m:], up[m:], hidden_grad)
        for c in range(4):
            lanes = slice(c * step, (c + 1) * step)
            part[s, 0, :, lanes] = jnp.dot(hidden_late, w[2, :, lanes], preferred_element_type=f32).astype(bf16)
            part[s, 1, :, lanes] = (
                jnp.dot(gate_grad, w[0, :, lanes], preferred_element_type=f32)
                + jnp.dot(up_grad, w[1, :, lanes], preferred_element_type=f32)
            ).astype(bf16)
            early = slots[s, 1, :, lanes]
            acc[0, :, lanes] += contract_first(gate_grad, early)
            acc[1, :, lanes] += contract_first(up_grad, early)
            acc[2, :, lanes] += contract_first(hidden_early, slots[s, 2, :, lanes])

    def trade(s):
        return remote(part.at[s, :, half(1 - t), :], peer.at[s], ts.at[s], tr.at[s], {"tp": 1 - t})

    def along(s, d):
        block = slots.at[s, :, quarter(t, d), :]
        return remote(block, slots.at[s + 1, :, quarter(t, d), :], ags.at[d, s], agr.at[d, s], {"fs": ahead[d]})

    def arrived(s, d):
        block = slots.at[s, :, quarter(t, d), :]
        return remote(block, block, ags.at[d, s - 1], agr.at[d, s - 1], {"fs": ahead[d]})

    def across(s, d, core):
        block = slots.at[s, :, quarter(core, d), :]
        return remote(block, block, aps.at[d, s - 1], apr.at[d, s - 1], {"tp": 1 - t})

    def ring_step(s, carry):
        for d in range(2):
            arrived(s, d).wait_recv()

            @pl.when(s < n - 1)
            def _():
                along(s, d).start()

            across(s, d, t).start()

        @pl.when(s > 1)
        def _():
            for d in range(2):
                across(s - 1, d, 1 - t).wait_recv()

        compute(s - 1)
        trade(s - 1).start()
        return carry

    lax.fori_loop(1, n, ring_step, 0)

    def own(s, o, d):
        return (
            part[s, o, quarter(t, d), :].astype(f32)
            + peer[s, o, d * q:(d + 1) * q, :].astype(f32)
        )

    def trade_done(s):
        remote(peer.at[s], peer.at[s], ts.at[s], tr.at[s], {"tp": 1 - t}).wait_recv()

    def sum_step(s):
        trade_done(s + 1)
        for o in range(2):
            for d in range(2):
                value = own(s + 1, o, d)
                if s > 0:
                    slot = ring_in.at[d, s - 1, o]
                    remote(slot, slot, rs.at[d, s - 1, o], rr.at[d, s - 1, o], {"fs": ahead[d]}).wait_recv()
                    value = value + ring_in[d, s - 1, o].astype(f32)
                ring_out[d, s, o] = value.astype(bf16)
                go(remote(ring_out.at[d, s, o], ring_in.at[d, s, o], rs.at[d, s, o], rr.at[d, s, o], {"fs": ahead[d]}))

    sum_step(0)
    for d in range(2):
        across(n - 1, d, 1 - t).wait_recv()
    compute(n - 1)
    trade(n - 1).start()
    grads[...] = acc[...].astype(bf16)
    order = list(range(1, n)) + [0]
    for k in order:
        g = lax.rem(f + k, n)
        go(remote(grads.at[:, :, span(g * dl + (1 - r) * hl, hl, hl)], x_in.at[k], xs.at[k], xr.at[k], {"rep": 1 - r}))

    def g_block(origin, side):
        return g_out.at[:, span(origin * hid, hid, hid), span(side * hl, hl, hl)]

    def pair_sum(k):
        g = lax.rem(f + k, n)
        remote(x_in.at[k], x_in.at[k], xs.at[k], xr.at[k], {"rep": 1 - r}).wait_recv()
        return (x_in[k].astype(f32) + acc[:, :, span(g * dl + r * hl, hl, hl)]).astype(bf16)

    def pass_on(k):
        origin = lax.rem(f - k + n, n)
        block = g_block(origin, r)
        remote(block, block, gs.at[k - 1], gr.at[k - 1], {"fs": origin}).wait_recv()
        go(remote(block, block, fs_.at[k], fr.at[k], {"rep": 1 - r}))

    for s in range(n - 1):
        if s > 0:
            sum_step(s)
        x_out[s] = pair_sum(s + 1)
        go(remote(x_out.at[s], g_block(f, r), gs.at[s], gr.at[s], {"fs": lax.rem(f + s + 1, n)}))
        if s >= 2:
            pass_on(s - 1)
    g_out[:, span(f * hid, hid, hid), span(r * hl, hl, hl)] = pair_sum(0)
    block = g_block(f, r)
    go(remote(block, block, fs_.at[0], fr.at[0], {"rep": 1 - r}))
    trade_done(0)
    for o in range(2):
        for d in range(2):
            slot = ring_in.at[d, n - 2, o]
            remote(slot, slot, rs.at[d, n - 2, o], rr.at[d, n - 2, o], {"fs": ahead[d]}).wait_recv()
            value = own(0, o, d) + ring_in[d, n - 2, o].astype(f32)
            outs[o][quarter(t, d), :] = value.astype(bf16)
        mine = outs[o].at[half(t), :]
        go(remote(mine, mine, os_.at[o], or_.at[o], {"tp": 1 - t}))
    for k in range(n - 2, n):
        pass_on(k)
    for o in range(2):
        other = outs[o].at[half(1 - t), :]
        remote(other, other, os_.at[o], or_.at[o], {"tp": 1 - t}).wait_recv()
    for k in range(n):
        block = g_block(lax.rem(f - k + n, n), 1 - r)
        remote(block, block, fs_.at[k], fr.at[k], {"rep": 1 - r}).wait_recv()
    for s in range(n):
        trade(s).wait_send()
    for s in range(1, n):
        for d in range(2):
            if s < n - 1:
                along(s, d).wait_send()
            across(s, d, t).wait_send()
    for copy in pending:
        copy.wait_send()


def add_kernel(total, first, second, third, first_new, second_new, third_new):
    for i, (old, new) in enumerate(((first, first_new), (second, second_new), (third, third_new))):
        new[...] = old[...] + total[i].astype(jnp.float32).T


def add_turned(total, sums):
    _, ff, dl = total.shape
    width = 256
    block = pl.BlockSpec((dl, width), lambda i: (0, i))
    return pl.pallas_call(
        add_kernel,
        grid=(ff // width,),
        out_shape=tuple(jax.ShapeDtypeStruct(old.shape, old.dtype) for old in sums),
        in_specs=[pl.BlockSpec((3, width, dl), lambda i: (0, i, 0))] + [block] * 3,
        out_specs=(block,) * 3,
        name="add_turned",
    )(total, *sums)


VMEM = pl.BlockSpec(memory_space=pltpu.VMEM)


def dma(*shape):
    return pltpu.SemaphoreType.DMA(shape)


def split_hidden(
    n,
    later_input,
    earlier_input,
    cotangent,
    gate_weight,
    up_weight,
    down_weight,
    gate_sum,
    up_sum,
    down_sum,
):
    bf16 = jnp.bfloat16
    m, width = later_input.shape
    dl, ff = gate_weight.shape
    hid = ff // n
    hl, q = dl // 2, m // 4
    tokens = jnp.stack([later_input, earlier_input, cotangent])
    weights = jnp.stack([gate_weight.T, up_weight.T, down_weight.T])
    later_output, earlier_input_grad, total = pl.pallas_call(
        functools.partial(fused_kernel, n),
        out_shape=(
            jax.ShapeDtypeStruct((m, width), bf16),
            jax.ShapeDtypeStruct((m, width), bf16),
            jax.ShapeDtypeStruct((3, ff, dl), bf16),
        ),
        in_specs=[VMEM] * 2,
        out_specs=(VMEM, VMEM, VMEM),
        scratch_shapes=[
            pltpu.VMEM((n, 3, m, width), bf16),
            pltpu.VMEM((3, hid, width), bf16),
            pltpu.VMEM((n, 2, m, width), bf16),
            pltpu.VMEM((n, 2, 2 * q, width), bf16),
            pltpu.VMEM((3, hid, width), jnp.float32),
            pltpu.VMEM((3, hid, width), bf16),
            pltpu.VMEM((2, n - 1, 2, q, width), bf16),
            pltpu.VMEM((2, n - 1, 2, q, width), bf16),
            pltpu.VMEM((n, 3, hid, hl), bf16),
            pltpu.VMEM((n - 1, 3, hid, hl), bf16),
        ]
        + [dma(2, n - 1)] * 4
        + [dma(n - 1)] * 4
        + [
            dma(n), dma(n),
            dma(2, n - 1, 2), dma(2, n - 1, 2),
            dma(2), dma(2),
            dma(n), dma(n),
            dma(n - 1), dma(n - 1),
            dma(n), dma(n),
        ],
        compiler_params=pltpu.CompilerParams(
            collective_id=0, has_side_effects=True, vmem_limit_bytes=67043328
        ),
        name="fused",
    )(tokens, weights)
    return (later_output, earlier_input_grad) + tuple(add_turned(total, (gate_sum, up_sum, down_sum)))


def early_parts(gate_early, up_early, hidden_grad):
    sigmoid_gate = jax.nn.sigmoid(gate_early)
    silu_early = gate_early * sigmoid_gate
    gate_grad = (
        hidden_grad * up_early * sigmoid_gate * (1.0 + gate_early * (1.0 - sigmoid_gate))
    ).astype(jnp.bfloat16)
    up_grad = (hidden_grad * silu_early).astype(jnp.bfloat16)
    hidden_early = (silu_early * up_early).astype(jnp.bfloat16)
    return gate_grad, up_grad, hidden_early


def contract_last(first, second):
    return lax.dot_general(
        first, second, (((1,), (1,)), ((), ())), preferred_element_type=jnp.float32
    )


def contract_first(first, second):
    return lax.dot_general(
        first, second, (((0,), (0,)), ((), ())), preferred_element_type=jnp.float32
    )


def per_device(
    later_input,
    earlier_input,
    cotangent,
    gate_weight,
    up_weight,
    down_weight,
    gate_sum,
    up_sum,
    down_sum,
):
    gate_full, up_full, down_full = (
        lax.all_gather(gate_weight, "fs", axis=0, tiled=True),
        lax.all_gather(up_weight, "fs", axis=0, tiled=True),
        lax.all_gather(down_weight, "fs", axis=0, tiled=True),
    )
    gate_late = jnp.dot(later_input, gate_full, preferred_element_type=jnp.float32)
    up_late = jnp.dot(later_input, up_full, preferred_element_type=jnp.float32)
    hidden_late = (jax.nn.silu(gate_late) * up_late).astype(jnp.bfloat16)
    partial_late = contract_last(hidden_late, down_full)
    later_output = lax.psum(partial_late.astype(jnp.bfloat16), "tp")
    gate_early = jnp.dot(earlier_input, gate_full, preferred_element_type=jnp.float32)
    up_early = jnp.dot(earlier_input, up_full, preferred_element_type=jnp.float32)
    hidden_grad = jnp.dot(cotangent, down_full, preferred_element_type=jnp.float32)
    sigmoid_gate = jax.nn.sigmoid(gate_early)
    silu_early = gate_early * sigmoid_gate
    gate_grad = (
        hidden_grad * up_early * sigmoid_gate * (1.0 + gate_early * (1.0 - sigmoid_gate))
    ).astype(jnp.bfloat16)
    up_grad = (hidden_grad * silu_early).astype(jnp.bfloat16)
    hidden_early = (silu_early * up_early).astype(jnp.bfloat16)
    partial_early = contract_last(gate_grad, gate_full) + contract_last(up_grad, up_full)
    earlier_input_grad = lax.psum(partial_early.astype(jnp.bfloat16), "tp")
    columns, cot_columns = (
        lax.all_to_all(earlier_input, "fs", split_axis=1, concat_axis=0, tiled=True),
        lax.all_to_all(cotangent, "fs", split_axis=1, concat_axis=0, tiled=True),
    )
    gate_local = contract_first(columns, lax.all_gather(gate_grad, "fs", axis=0, tiled=True))
    up_local = contract_first(columns, lax.all_gather(up_grad, "fs", axis=0, tiled=True))
    down_local = contract_first(cot_columns, lax.all_gather(hidden_early, "fs", axis=0, tiled=True))
    gate_total, up_total, down_total = (
        lax.psum(gate_local.astype(jnp.bfloat16), "rep").astype(jnp.float32),
        lax.psum(up_local.astype(jnp.bfloat16), "rep").astype(jnp.float32),
        lax.psum(down_local.astype(jnp.bfloat16), "rep").astype(jnp.float32),
    )
    return (
        later_output,
        earlier_input_grad,
        gate_sum + gate_total,
        up_sum + up_total,
        down_sum + down_total,
    )


def solution(mesh):
    placed = (
        P(("rep", "fs"), None),
        P(("rep", "fs"), None),
        P(("rep", "fs"), None),
        P("fs", "tp"),
        P("fs", "tp"),
        P("fs", "tp"),
        P("fs", "tp"),
        P("fs", "tp"),
        P("fs", "tp"),
    )
    reps, shards, blocks = (mesh.shape[axis] for axis in ("rep", "fs", "tp"))

    def chosen(*arrays):
        rows = arrays[0].shape[0]
        depth, units = arrays[3].shape
        fits = (
            reps == 2
            and blocks == 2
            and shards % 2 == 0
            and units % (shards * 16) == 0
            and depth % 256 == 0
            and rows % 64 == 0
            and units % 256 == 0
            and arrays[0].shape[1] % 512 == 0
        )
        return split_hidden(shards, *arrays) if fits else per_device(*arrays)

    return jax.shard_map(
        chosen,
        mesh=mesh,
        in_specs=placed,
        out_specs=(
            P(("rep", "fs"), None),
            P(("rep", "fs"), None),
            P("fs", "tp"),
            P("fs", "tp"),
            P("fs", "tp"),
        ),
        check_vma=False,
    )
```

```python
import functools

import jax
import jax.numpy as jnp
from jax import lax
from jax.experimental import pallas as pl
from jax.experimental.pallas import tpu as pltpu
from jax.sharding import PartitionSpec as P

MESH = pl.DeviceIdType.MESH


def ring_position(index, n):
    side, height = lax.rem(index, 2), index // 2
    return (1 - side) * height + side * (n - 1 - height)


def ring_index(position, n):
    position = lax.rem(position + 2 * n, n)
    back = position // (n // 2)
    return (1 - back) * (2 * position) + back * (2 * (n - 1 - position) + 1)


def span(start, size, step):
    return pl.ds(pl.multiple_of(start, step), size)


def remote(source, target, send, recv, device):
    return pltpu.make_async_remote_copy(
        src_ref=source,
        dst_ref=target,
        send_sem=send,
        recv_sem=recv,
        device_id=device,
        device_id_type=MESH,
    )


def meet(n, r, f, t):
    barrier = pltpu.get_barrier_semaphore()
    for k in range(1, n):
        pl.semaphore_signal(barrier, inc=1, device_id={"fs": lax.rem(f + k, n)}, device_id_type=MESH)
    pl.semaphore_signal(barrier, inc=1, device_id={"rep": 1 - r}, device_id_type=MESH)
    pl.semaphore_signal(barrier, inc=1, device_id={"tp": 1 - t}, device_id_type=MESH)
    pl.semaphore_wait(barrier, n + 1)


def fused_kernel(
    n, tok, wt, late_out, early_out, g_out,
    slots, w, part, peer, acc, grads, ring_in, ring_out, x_in, x_out,
    ags, agr, aps, apr, ws, wr, wxs, wxr,
    ts, tr, rs, rr, os_, or_, xs, xr, gs, gr, fs_, fr,
):
    r, f, t = lax.axis_index("rep"), lax.axis_index("fs"), lax.axis_index("tp")
    m = tok.shape[1]
    q = m // 4
    hid, dl = wt.shape[1] // n, wt.shape[2]
    hl = dl // 2
    width = tok.shape[2]
    pos = ring_position(f, n)
    ahead = (ring_index(pos + 1, n), ring_index(pos - 1, n))
    outs = (late_out, early_out)
    f32, bf16 = jnp.float32, jnp.bfloat16
    meet(n, r, f, t)

    pending = []

    def go(copy):
        copy.start()
        pending.append(copy)

    def quarter(core, d):
        return span(core * (2 * q) + d * q, q, q)

    def half(core):
        return span(core * (2 * q), 2 * q, 2 * q)

    def piece(origin, side):
        return w.at[:, :, span(origin * dl + side * hl, hl, hl)]

    def along(s, d):
        block = slots.at[s, :, quarter(t, d), :]
        return remote(block, slots.at[s + 1, :, quarter(t, d), :], ags.at[d, s], agr.at[d, s], {"fs": ahead[d]})

    def arrived(s, d):
        block = slots.at[s, :, quarter(t, d), :]
        return remote(block, block, ags.at[d, s - 1], agr.at[d, s - 1], {"fs": ahead[d]})

    def across(s, d, core):
        block = slots.at[s, :, quarter(core, d), :]
        return remote(block, block, aps.at[d, s - 1], apr.at[d, s - 1], {"tp": 1 - t})

    def take_on(s):
        for d in range(2):
            arrived(s, d).wait_recv()

            @pl.when(s < n - 1)
            def _():
                along(s, d).start()

            across(s, d, t).start()

    for k in range(1, n):
        g = lax.rem(f + k, n)
        go(remote(
            wt.at[:, span(g * hid, hid, hid), span(r * hl, hl, hl)],
            piece(f, r), ws.at[k - 1], wr.at[k - 1], {"fs": g},
        ))
    for d in range(2):
        go(remote(tok.at[:, quarter(t, d), :], slots.at[1, :, quarter(t, d), :], ags.at[d, 0], agr.at[d, 0], {"fs": ahead[d]}))
    slots[0] = tok[...]
    w[:, :, span(f * dl, dl, dl)] = wt[:, span(f * hid, hid, hid), :]
    acc[...] = jnp.zeros_like(acc)
    for k in range(1, n):
        origin = lax.rem(f - k + n, n)
        block = piece(origin, r)
        remote(block, block, ws.at[k - 1], wr.at[k - 1], {"fs": origin}).wait_recv()
        go(remote(block, block, wxs.at[k - 1], wxr.at[k - 1], {"rep": 1 - r}))
    take_on(1)
    for k in range(1, n):
        block = piece(lax.rem(f - k + n, n), 1 - r)
        remote(block, block, wxs.at[k - 1], wxr.at[k - 1], {"rep": 1 - r}).wait_recv()

    step = width // 4

    def compute(s):
        pair = slots[s, 0:2].reshape(2 * m, width)
        gate, up = contract_last(pair, w[0]), contract_last(pair, w[1])
        hidden_late = (jax.nn.silu(gate[:m]) * up[:m]).astype(bf16)
        hidden_grad = contract_last(slots[s, 2], w[2])
        gate_grad, up_grad, hidden_early = early_parts(gate[m:], up[m:], hidden_grad)
        for c in range(4):
            lanes = slice(c * step, (c + 1) * step)
            part[s, 0, :, lanes] = jnp.dot(hidden_late, w[2, :, lanes], preferred_element_type=f32).astype(bf16)
            part[s, 1, :, lanes] = (
                jnp.dot(gate_grad, w[0, :, lanes], preferred_element_type=f32)
                + jnp.dot(up_grad, w[1, :, lanes], preferred_element_type=f32)
            ).astype(bf16)
            early = slots[s, 1, :, lanes]
            acc[0, :, lanes] += contract_first(gate_grad, early)
            acc[1, :, lanes] += contract_first(up_grad, early)
            acc[2, :, lanes] += contract_first(hidden_early, slots[s, 2, :, lanes])

    def trade(s):
        return remote(part.at[s, :, half(1 - t), :], peer.at[s], ts.at[s], tr.at[s], {"tp": 1 - t})

    def ring_step(s, carry):
        @pl.when(s > 1)
        def _():
            take_on(s)

        @pl.when(s > 1)
        def _():
            for d in range(2):
                across(s - 1, d, 1 - t).wait_recv()

        compute(s - 1)
        trade(s - 1).start()
        return carry

    lax.fori_loop(1, n, ring_step, 0)

    def own(s, o, d):
        return (
            part[s, o, quarter(t, d), :].astype(f32)
            + peer[s, o, d * q:(d + 1) * q, :].astype(f32)
        )

    def trade_done(s):
        remote(peer.at[s], peer.at[s], ts.at[s], tr.at[s], {"tp": 1 - t}).wait_recv()

    def sum_step(s):
        trade_done(s + 1)
        for o in range(2):
            for d in range(2):
                value = own(s + 1, o, d)
                if s > 0:
                    slot = ring_in.at[d, s - 1, o]
                    remote(slot, slot, rs.at[d, s - 1, o], rr.at[d, s - 1, o], {"fs": ahead[d]}).wait_recv()
                    value = value + ring_in[d, s - 1, o].astype(f32)
                ring_out[d, s, o] = value.astype(bf16)
                go(remote(ring_out.at[d, s, o], ring_in.at[d, s, o], rs.at[d, s, o], rr.at[d, s, o], {"fs": ahead[d]}))

    sum_step(0)
    for d in range(2):
        across(n - 1, d, 1 - t).wait_recv()
    compute(n - 1)
    trade(n - 1).start()
    grads[...] = acc[...].astype(bf16)
    order = list(range(1, n)) + [0]
    for k in order:
        g = lax.rem(f + k, n)
        go(remote(grads.at[:, :, span(g * dl + (1 - r) * hl, hl, hl)], x_in.at[k], xs.at[k], xr.at[k], {"rep": 1 - r}))

    def g_block(origin, side):
        return g_out.at[:, span(origin * hid, hid, hid), span(side * hl, hl, hl)]

    def pair_sum(k):
        g = lax.rem(f + k, n)
        remote(x_in.at[k], x_in.at[k], xs.at[k], xr.at[k], {"rep": 1 - r}).wait_recv()
        return (x_in[k].astype(f32) + acc[:, :, span(g * dl + r * hl, hl, hl)]).astype(bf16)

    def pass_on(k):
        origin = lax.rem(f - k + n, n)
        block = g_block(origin, r)
        remote(block, block, gs.at[k - 1], gr.at[k - 1], {"fs": origin}).wait_recv()
        go(remote(block, block, fs_.at[k], fr.at[k], {"rep": 1 - r}))

    for s in range(n - 1):
        if s > 0:
            sum_step(s)
        x_out[s] = pair_sum(s + 1)
        go(remote(x_out.at[s], g_block(f, r), gs.at[s], gr.at[s], {"fs": lax.rem(f + s + 1, n)}))
        if s >= 1:
            pass_on(s)
    g_out[:, span(f * hid, hid, hid), span(r * hl, hl, hl)] = pair_sum(0)
    block = g_block(f, r)
    go(remote(block, block, fs_.at[0], fr.at[0], {"rep": 1 - r}))
    trade_done(0)
    for o in range(2):
        for d in range(2):
            slot = ring_in.at[d, n - 2, o]
            remote(slot, slot, rs.at[d, n - 2, o], rr.at[d, n - 2, o], {"fs": ahead[d]}).wait_recv()
            value = own(0, o, d) + ring_in[d, n - 2, o].astype(f32)
            outs[o][quarter(t, d), :] = value.astype(bf16)
        mine = outs[o].at[half(t), :]
        go(remote(mine, mine, os_.at[o], or_.at[o], {"tp": 1 - t}))
    for k in range(n - 1, n):
        pass_on(k)
    for o in range(2):
        other = outs[o].at[half(1 - t), :]
        remote(other, other, os_.at[o], or_.at[o], {"tp": 1 - t}).wait_recv()
    for k in range(n):
        block = g_block(lax.rem(f - k + n, n), 1 - r)
        remote(block, block, fs_.at[k], fr.at[k], {"rep": 1 - r}).wait_recv()
    for s in range(n):
        trade(s).wait_send()
    for s in range(1, n):
        for d in range(2):
            if s < n - 1:
                along(s, d).wait_send()
            across(s, d, t).wait_send()
    for copy in pending:
        copy.wait_send()


def add_kernel(total, first, second, third, first_new, second_new, third_new):
    for i, (old, new) in enumerate(((first, first_new), (second, second_new), (third, third_new))):
        new[...] = old[...] + total[i].astype(jnp.float32).T


def add_turned(total, sums):
    _, ff, dl = total.shape
    width = 256
    block = pl.BlockSpec((dl, width), lambda i: (0, i))
    return pl.pallas_call(
        add_kernel,
        grid=(ff // width,),
        out_shape=tuple(jax.ShapeDtypeStruct(old.shape, old.dtype) for old in sums),
        in_specs=[pl.BlockSpec((3, width, dl), lambda i: (0, i, 0))] + [block] * 3,
        out_specs=(block,) * 3,
        name="add_turned",
    )(total, *sums)


VMEM = pl.BlockSpec(memory_space=pltpu.VMEM)


def dma(*shape):
    return pltpu.SemaphoreType.DMA(shape)


def split_hidden(
    n,
    later_input,
    earlier_input,
    cotangent,
    gate_weight,
    up_weight,
    down_weight,
    gate_sum,
    up_sum,
    down_sum,
):
    bf16 = jnp.bfloat16
    m, width = later_input.shape
    dl, ff = gate_weight.shape
    hid = ff // n
    hl, q = dl // 2, m // 4
    tokens = jnp.stack([later_input, earlier_input, cotangent])
    weights = jnp.stack([gate_weight.T, up_weight.T, down_weight.T])
    later_output, earlier_input_grad, total = pl.pallas_call(
        functools.partial(fused_kernel, n),
        out_shape=(
            jax.ShapeDtypeStruct((m, width), bf16),
            jax.ShapeDtypeStruct((m, width), bf16),
            jax.ShapeDtypeStruct((3, ff, dl), bf16),
        ),
        in_specs=[VMEM] * 2,
        out_specs=(VMEM, VMEM, VMEM),
        scratch_shapes=[
            pltpu.VMEM((n, 3, m, width), bf16),
            pltpu.VMEM((3, hid, width), bf16),
            pltpu.VMEM((n, 2, m, width), bf16),
            pltpu.VMEM((n, 2, 2 * q, width), bf16),
            pltpu.VMEM((3, hid, width), jnp.float32),
            pltpu.VMEM((3, hid, width), bf16),
            pltpu.VMEM((2, n - 1, 2, q, width), bf16),
            pltpu.VMEM((2, n - 1, 2, q, width), bf16),
            pltpu.VMEM((n, 3, hid, hl), bf16),
            pltpu.VMEM((n - 1, 3, hid, hl), bf16),
        ]
        + [dma(2, n - 1)] * 4
        + [dma(n - 1)] * 4
        + [
            dma(n), dma(n),
            dma(2, n - 1, 2), dma(2, n - 1, 2),
            dma(2), dma(2),
            dma(n), dma(n),
            dma(n - 1), dma(n - 1),
            dma(n), dma(n),
        ],
        compiler_params=pltpu.CompilerParams(
            collective_id=0, has_side_effects=True, vmem_limit_bytes=67043328
        ),
        name="fused",
    )(tokens, weights)
    return (later_output, earlier_input_grad) + tuple(add_turned(total, (gate_sum, up_sum, down_sum)))


def early_parts(gate_early, up_early, hidden_grad):
    sigmoid_gate = jax.nn.sigmoid(gate_early)
    silu_early = gate_early * sigmoid_gate
    gate_grad = (
        hidden_grad * up_early * sigmoid_gate * (1.0 + gate_early * (1.0 - sigmoid_gate))
    ).astype(jnp.bfloat16)
    up_grad = (hidden_grad * silu_early).astype(jnp.bfloat16)
    hidden_early = (silu_early * up_early).astype(jnp.bfloat16)
    return gate_grad, up_grad, hidden_early


def contract_last(first, second):
    return lax.dot_general(
        first, second, (((1,), (1,)), ((), ())), preferred_element_type=jnp.float32
    )


def contract_first(first, second):
    return lax.dot_general(
        first, second, (((0,), (0,)), ((), ())), preferred_element_type=jnp.float32
    )


def per_device(
    later_input,
    earlier_input,
    cotangent,
    gate_weight,
    up_weight,
    down_weight,
    gate_sum,
    up_sum,
    down_sum,
):
    gate_full, up_full, down_full = (
        lax.all_gather(gate_weight, "fs", axis=0, tiled=True),
        lax.all_gather(up_weight, "fs", axis=0, tiled=True),
        lax.all_gather(down_weight, "fs", axis=0, tiled=True),
    )
    gate_late = jnp.dot(later_input, gate_full, preferred_element_type=jnp.float32)
    up_late = jnp.dot(later_input, up_full, preferred_element_type=jnp.float32)
    hidden_late = (jax.nn.silu(gate_late) * up_late).astype(jnp.bfloat16)
    partial_late = contract_last(hidden_late, down_full)
    later_output = lax.psum(partial_late.astype(jnp.bfloat16), "tp")
    gate_early = jnp.dot(earlier_input, gate_full, preferred_element_type=jnp.float32)
    up_early = jnp.dot(earlier_input, up_full, preferred_element_type=jnp.float32)
    hidden_grad = jnp.dot(cotangent, down_full, preferred_element_type=jnp.float32)
    sigmoid_gate = jax.nn.sigmoid(gate_early)
    silu_early = gate_early * sigmoid_gate
    gate_grad = (
        hidden_grad * up_early * sigmoid_gate * (1.0 + gate_early * (1.0 - sigmoid_gate))
    ).astype(jnp.bfloat16)
    up_grad = (hidden_grad * silu_early).astype(jnp.bfloat16)
    hidden_early = (silu_early * up_early).astype(jnp.bfloat16)
    partial_early = contract_last(gate_grad, gate_full) + contract_last(up_grad, up_full)
    earlier_input_grad = lax.psum(partial_early.astype(jnp.bfloat16), "tp")
    columns, cot_columns = (
        lax.all_to_all(earlier_input, "fs", split_axis=1, concat_axis=0, tiled=True),
        lax.all_to_all(cotangent, "fs", split_axis=1, concat_axis=0, tiled=True),
    )
    gate_local = contract_first(columns, lax.all_gather(gate_grad, "fs", axis=0, tiled=True))
    up_local = contract_first(columns, lax.all_gather(up_grad, "fs", axis=0, tiled=True))
    down_local = contract_first(cot_columns, lax.all_gather(hidden_early, "fs", axis=0, tiled=True))
    gate_total, up_total, down_total = (
        lax.psum(gate_local.astype(jnp.bfloat16), "rep").astype(jnp.float32),
        lax.psum(up_local.astype(jnp.bfloat16), "rep").astype(jnp.float32),
        lax.psum(down_local.astype(jnp.bfloat16), "rep").astype(jnp.float32),
    )
    return (
        later_output,
        earlier_input_grad,
        gate_sum + gate_total,
        up_sum + up_total,
        down_sum + down_total,
    )


def solution(mesh):
    placed = (
        P(("rep", "fs"), None),
        P(("rep", "fs"), None),
        P(("rep", "fs"), None),
        P("fs", "tp"),
        P("fs", "tp"),
        P("fs", "tp"),
        P("fs", "tp"),
        P("fs", "tp"),
        P("fs", "tp"),
    )
    reps, shards, blocks = (mesh.shape[axis] for axis in ("rep", "fs", "tp"))

    def chosen(*arrays):
        rows = arrays[0].shape[0]
        depth, units = arrays[3].shape
        fits = (
            reps == 2
            and blocks == 2
            and shards % 2 == 0
            and units % (shards * 16) == 0
            and depth % 256 == 0
            and rows % 64 == 0
            and units % 256 == 0
            and arrays[0].shape[1] % 512 == 0
        )
        return split_hidden(shards, *arrays) if fits else per_device(*arrays)

    return jax.shard_map(
        chosen,
        mesh=mesh,
        in_specs=placed,
        out_specs=(
            P(("rep", "fs"), None),
            P(("rep", "fs"), None),
            P("fs", "tp"),
            P("fs", "tp"),
            P("fs", "tp"),
        ),
        check_vma=False,
    )
```
